32 devices in a mesh: fs: 16 (over z, y, x), tp: 2 (over core).
Axes of the slice: x: 2, y: 2, z: 4, core: 2. Of those that a mesh axis runs over, the one named last changes fastest.
Arguments:
- tokens: bfloat16 [12288, 2048], P('fs'), may hold values from -6 to 6
- norm_gain: float32 [2048], replicated, may hold values from 0.1 to 1.9
- up_weight: float32 [2048, 8192], P('fs', 'tp'), may hold values from -0.125 to 0.125
- up_scale: float32 [8192], P('tp'), may hold values from 0.5 to 2
- down_weight: float32 [8192, 2048], P('tp', 'fs'), may hold values from -0.0625 to 0.0625
- down_scale: float32 [2048], P('fs'), may hold values from 0.5 to 2
Outputs:
- output: bfloat16 [12288, 2048], P('fs', 'tp')
The draws below stay inside these ranges and needn't reach their ends.
All inputs are finite; a program needn't handle non-finite values.
Results may differ from the reference program's by a relative error of at most 0.015.
Values may be sent and summed in bfloat16 or wider, within the bound.
A program may use at most 128 MiB of HBM per device.

```python
import math
import jax
import jax.numpy as jnp
from jax import lax

D = 2048
FF = 8192
TOKENS = 12288
N_TP = 2


def level_of(stream_key, dims, split, least, high):
    def one(axis_at, shards_of):
        steps = jax.random.uniform(jax.random.fold_in(jax.random.fold_in(stream_key, 6), axis_at), (shards_of,), jnp.float32, least / len(split), high / len(split))
        return jnp.repeat(jnp.exp(steps), dims[axis_at] // shards_of).reshape((-1,) + (1,) * (len(dims) - axis_at - 1))

    factor_of = one(*split[0])
    for cut in split[1:]:
        factor_of = factor_of * one(*cut)
    return factor_of


def scatter_about(rng, dims, deviation, most, pieces=(), kind=jnp.bfloat16):
    level = level_of(rng, dims, pieces, -0.22, 0.18) if pieces else 1.0
    drawn = jax.random.normal(rng, dims, jnp.float32) * deviation * level
    return jnp.minimum(jnp.maximum(drawn, -most), most).astype(kind)


def setup_inputs(seed: int = 0) -> dict:
    seeds = jax.random.split(jax.random.key(seed), 7)
    return {
        "tokens": scatter_about(seeds[0], (TOKENS, D), 1.0, 6.0, ((0, 16),)),
        "norm_gain": jnp.clip(1.0 + 0.18 * jax.random.normal(seeds[1], (D,), jnp.float32), 0.1, 1.9),
        "up_weight": scatter_about(seeds[2], (D, FF), D ** -0.5, 0.125, ((0, 16), (1, 2)), jnp.float32),
        "up_scale": jnp.clip(jnp.exp(math.log(2.0) - 1.3862944 * jax.random.uniform(seeds[3], (FF,), jnp.float32) ** level_of(seeds[3], (FF,), ((0, 2),), -0.2, 0.2)), 0.5, 2.0),
        "down_weight": scatter_about(seeds[4], (FF, D), FF ** -0.5, 0.0625, ((0, 2), (1, 16)), jnp.float32),
        "down_scale": jnp.clip(jnp.exp(math.log(2.0) - 1.3862944 * jax.random.uniform(seeds[5], (D,), jnp.float32) ** level_of(seeds[5], (D,), ((0, 16),), -0.2, 0.2)), 0.5, 2.0),
    }


epsilon = 1e-06

def reference(tokens, norm_gain, up_weight, up_scale, down_weight, down_scale):
    floats = tokens.astype(jnp.float32)
    inverse = lax.rsqrt(lax.optimization_barrier(jnp.mean(floats * floats, axis=-1, keepdims=True)) + epsilon)
    normed = (floats * inverse * norm_gain).astype(jnp.bfloat16)
    up_half = up_weight.astype(jnp.bfloat16)
    down_half = down_weight.astype(jnp.bfloat16)
    up_pre = jnp.dot(normed, up_half, preferred_element_type=jnp.float32) * up_scale
    hidden = jnp.square(jax.nn.relu(up_pre)).astype(jnp.bfloat16)
    block_width = FF // N_TP
    summed = jnp.zeros((tokens.shape[0], D), jnp.float32)
    for block in range(N_TP):
        lower = block * block_width
        partial_value = jnp.dot(hidden[:, lower:lower + block_width], down_half[lower:lower + block_width], preferred_element_type=jnp.float32).astype(jnp.bfloat16)
        summed = summed + partial_value.astype(jnp.float32)
    return (summed * down_scale).astype(jnp.bfloat16)
```

```python
import jax
import jax.numpy as jnp
from jax import lax
from jax.experimental import pallas as pl
from jax.experimental.pallas import tpu as pltpu
from jax.sharding import PartitionSpec as P

epsilon = 1e-06


def normalise(tokens, norm_gain):
    floats = tokens.astype(jnp.float32)
    inverse = lax.rsqrt(jnp.mean(floats * floats, axis=-1, keepdims=True) + epsilon)
    return (floats * inverse * norm_gain).astype(jnp.bfloat16)


def plain(tokens, norm_gain, up_weight, up_scale, down_weight, down_scale):
    normed = normalise(tokens, norm_gain)
    up_whole = lax.all_gather(up_weight.astype(jnp.bfloat16), "fs", axis=0, tiled=True)
    up_pre = jnp.dot(normed, up_whole, preferred_element_type=jnp.float32)
    scaled = (down_weight * down_scale).astype(jnp.bfloat16)
    down_whole = lax.all_gather(scaled, "fs", axis=1, tiled=True)
    hidden = jnp.square(jax.nn.relu(up_pre * up_scale)).astype(jnp.bfloat16)
    partial_value = jnp.dot(hidden, down_whole, preferred_element_type=jnp.float32)
    return lax.psum_scatter(
        partial_value.astype(jnp.bfloat16), "tp", scatter_dimension=1, tiled=True
    )


NX, NY = 2, 2
order = (0, 1, 3, 2)


def kernel(tok_ref, gain_ref, s_ref, up_ref, down_ref, dscale_ref, out_ref,
           x_buf, u_in, d_in, u_send, d_send, u_buf, d_buf, t_buf, h_buf, ssend, srecv,
           xsend, xrecv, keep, part, send_sems, recv_sems, local_sems):
    me = lax.axis_index("fs")
    c = lax.axis_index("tp")
    x = lax.rem(me, NX)
    y = lax.rem(me // NX, NY)
    z = me // (NX * NY)
    side = lax.rem(z, 2)
    rows = x_buf.shape[0]
    depth = u_send.shape[0]
    wide = u_send.shape[1]
    cols = d_send.shape[1]
    pair = NX * cols
    part_rows = rows // 2

    def fs_of(zz, yy, xx):
        return (zz * NY + yy) * NX + xx

    def level(k):
        return {0: z, 1: z + 1 - 2 * side, 2: lax.rem(z + 2, 4), 3: 3 - z}[k]

    target = {
        **{k: {"fs": fs_of(level(k), y, x), "tp": c} for k in (1, 2, 3)},
        "y": {"fs": fs_of(z, 1 - y, x), "tp": c},
        "x": {"fs": fs_of(z, y, 1 - x), "tp": c},
        "c": {"fs": me, "tp": 1 - c},
    }
    peer = 1

    mine_rows = pl.ds(pl.multiple_of(c * part_rows, part_rows), part_rows)
    other_rows = pl.ds(pl.multiple_of((1 - c) * part_rows, part_rows), part_rows)
    local = [
        pltpu.make_async_copy(up_ref, u_in, local_sems.at[0]),
        pltpu.make_async_copy(tok_ref, x_buf, local_sems.at[1]),
        pltpu.make_async_copy(down_ref, d_in, local_sems.at[2]),
    ]
    for copy in local:
        copy.start()

    barrier = pltpu.get_barrier_semaphore()
    for where in target.values():
        pl.semaphore_signal(barrier, inc=1, device_id=where, device_id_type=pl.DeviceIdType.MESH)

    slots, started = {}, []

    def copy_of(key, src, dst, way):
        n = slots.setdefault(key, len(slots))
        return pltpu.make_async_remote_copy(
            src_ref=src, dst_ref=dst, send_sem=send_sems.at[n], recv_sem=recv_sems.at[n],
            device_id=target[way], device_id_type=pl.DeviceIdType.MESH)

    def launch(key, src, dst, way):
        copy = copy_of(key, src, dst, way)
        copy.start()
        started.append(copy)

    def arrive(key, dst, way="x"):
        copy_of(key, dst, dst, way).wait_recv()

    def block(kind, k, px, py, half=None):
        zz, yy = level(k), lax.rem(y + py, NY)
        xx = lax.rem(x + px, NX)
        if kind == "U":
            size = depth if half is None else depth // 2
            at = fs_of(zz, yy, xx) * depth + (0 if half in (None, 0) else size)
            return u_buf.at[pl.ds(pl.multiple_of(at, size), size), :]
        size = wide if half is None else wide // 2
        at = 0 if half in (None, 0) else size
        return d_buf.at[zz * NY + yy, pl.ds(at, size), pl.ds(pl.multiple_of(xx * cols, cols), cols)]

    own = {kind: block(kind, 0, 0, 0) for kind in "UD"}
    other = {"U": u_send, "D": d_send}

    def column(kind, k):
        launch((kind, k, 0, 0, None), own[kind] if k == 2 else other[kind], own[kind], k)

    def take(kind, k, px, py, half=None):
        arrive((kind, k, px, py, half), block(kind, k, px, py, half))

    def share(kind, k):
        if k:
            take(kind, k, 0, 0)
        ref = block(kind, k, 0, 0)
        launch((kind, k, 1, 0, None), ref, ref, "x")
        launch((kind, k, 0, 1, None), ref, ref, "y")

    def cross(kind, k):
        for px, py, way, half in ((1, 0, "y", 0), (0, 1, "x", 1)):
            take(kind, k, px, py)
            ref = block(kind, k, px, py, half)
            launch((kind, k, 1, 1, half), ref, ref, way)

    def corner(kind, k):
        take(kind, k, 1, 1, 0)
        take(kind, k, 1, 1, 1)

    at_own = pl.ds(pl.multiple_of(side * wide, wide), wide)
    at_other = pl.ds(pl.multiple_of((1 - side) * wide, wide), wide)

    local[0].wait()
    u_send[...] = u_in[:, at_other].astype(jnp.bfloat16)
    own["U"][...] = u_in[:, at_own].astype(jnp.bfloat16)
    pl.semaphore_wait(barrier, len(target))
    column("U", 1)
    share("U", 0)
    column("U", 3)
    column("U", 2)

    local[2].wait()
    d_send[...] = (d_in[at_other, :] * dscale_ref[...]).astype(jnp.bfloat16)
    own["D"][...] = (d_in[at_own, :] * dscale_ref[...]).astype(jnp.bfloat16)

    step = 16

    def normalise_rows(base):
        @pl.loop(0, part_rows // step)
        def _(i):
            r = pl.ds(pl.multiple_of(base + i * step, step), step)
            floats = x_buf[r, :].astype(jnp.float32)
            inverse = lax.rsqrt(jnp.mean(floats * floats, axis=-1, keepdims=True) + epsilon)
            x_buf[r, :] = (floats * inverse * gain_ref[...]).astype(jnp.bfloat16)

    local[1].wait()
    normalise_rows(c * part_rows)
    column("D", 1)
    column("D", 3)
    launch(("T", "x"), x_buf.at[mine_rows, :], t_buf.at[mine_rows, :], peer)
    column("D", 2)
    normalise_rows((1 - c) * part_rows)

    share("U", 1)
    cross("U", 0)
    cross("U", 1)
    share("U", 3)
    share("U", 2)
    cross("U", 3)
    cross("U", 2)
    share("D", 0)
    share("D", 1)
    for k in order:
        corner("U", k)

    tile_m, tile_n = part_rows, min(512, wide)
    chunks = wide // tile_n

    def up_part(src, base, first, count, jfirst=0, jcount=chunks):
        @pl.loop(jfirst, jfirst + jcount)
        def _(j):
            at = pl.ds(pl.multiple_of(j * tile_n, tile_n), tile_n)
            at_s = pl.ds(pl.multiple_of(side * wide + j * tile_n, tile_n), tile_n)

            for i in range(count):
                r = pl.multiple_of(first + i * tile_m, tile_m)
                pre = jnp.dot(src[pl.ds(r, tile_m), :], u_buf[:, at],
                              preferred_element_type=jnp.float32)
                act = jnp.square(jnp.maximum(pre * s_ref[:, at_s], 0.0))
                h_buf[pl.ds(base + r, tile_m), at] = act.astype(jnp.bfloat16)

    up_part(x_buf, 0, 0, 2)
    cross("D", 0)
    arrive(("T", "x"), t_buf.at[mine_rows, :])
    launch(("T", "c"), t_buf.at[mine_rows, :], t_buf.at[mine_rows, :], "c")
    cross("D", 1)
    up_part(t_buf, rows, c * part_rows, 1)
    share("D", 3)
    arrive(("T", "c"), t_buf.at[other_rows, :])
    up_part(t_buf, rows, (1 - c) * part_rows, 1)

    span = rows // 2

    def dots(base, zy, put):
        @pl.loop(0, rows // span)
        def _(i):
            r = pl.multiple_of(i * span, span)
            put(pl.ds(r, span), jnp.dot(h_buf[pl.ds(base + r, span), :], d_buf[zy],
                                        preferred_element_type=jnp.float32))

    finals = []

    def stage(k, py):
        j = order.index(k)
        zz, yy = level(k), lax.rem(y + py, NY)
        zy = zz * NY + yy
        n = (j % 2) * 2 + py
        met = (n + 2) % 4
        mine = zz // 2 == c

        @pl.when(jnp.logical_not(mine))
        def _():
            for half, base in ((0, rows), (1, 0)):
                ref = ssend.at[n, half]

                def put(r, value):
                    ssend[n, half, r, :] = value.astype(jnp.bfloat16)

                dots(base, zy, put)
                copy_of(("S", n, half), ref, srecv.at[n, half], "c").start()

        @pl.when(mine)
        def _():
            def put(r, value):
                part[r, :] = value

            dots(rows, zy, put)
            arrive(("S", n, 0), srecv.at[n, 0])
            xsend[n] = (part[...] + srecv[n, 0].astype(jnp.float32)).astype(jnp.bfloat16)
            copy_of(("X", met), xsend.at[n], xrecv.at[met], peer).start()

            def put_keep(r, value):
                keep[n, r, :] = value

            dots(0, zy, put_keep)
            arrive(("S", n, 1), srecv.at[n, 1])
            keep[n] = keep[n] + srecv[n, 1].astype(jnp.float32)

    def finish(k, py):
        j = order.index(k)
        zz, yy = level(k), lax.rem(y + py, NY)
        n = (j % 2) * 2 + py
        met = (n + 2) % 4

        @pl.when(zz // 2 == c)
        def _():
            arrive(("X", n), xrecv.at[n])
            at = pl.multiple_of((lax.rem(zz, 2) * NY + yy) * pair, pair)
            out_ref[:, pl.ds(at, pair)] = (keep[n] + xrecv[n].astype(jnp.float32)).astype(out_ref.dtype)
            copy_of(("X", met), xsend.at[n], xrecv.at[met], peer).wait_send()

        @pl.when(zz // 2 != c)
        def _():
            for half in range(2):
                copy_of(("S", n, half), ssend.at[n, half], srecv.at[n, half], "c").wait_send()

    stage(0, 0)
    corner("D", 0)
    stage(0, 1)
    share("D", 2)
    stage(1, 0)
    corner("D", 1)
    stage(1, 1)
    cross("D", 3)
    stage(3, 0)
    cross("D", 2)
    stage(2, 0)
    for py in range(2):
        finish(0, py)
        finish(1, py)
    corner("D", 3)
    stage(3, 1)
    corner("D", 2)
    stage(2, 1)
    for k, py in ((3, 0), (2, 0), (3, 1), (2, 1)):
        finish(k, py)
    for copy in started:
        copy.wait_send()


def fused(tokens, norm_gain, up_weight, up_scale, down_weight, down_scale):
    rows, width = tokens.shape
    depth, hidden = up_weight.shape
    cols = down_weight.shape[1]
    wide = hidden // 2
    nz = 4
    pair = NX * cols
    ways = 2 * (nz - 1 + 4 * nz) + 2 + 12
    vmem = pl.BlockSpec(memory_space=pltpu.VMEM)
    hbm = pl.BlockSpec(memory_space=pl.ANY)
    return pl.pallas_call(
        kernel,
        out_shape=jax.ShapeDtypeStruct((rows, width // 2), jnp.bfloat16),
        in_specs=[hbm, vmem, vmem, hbm, hbm, vmem],
        out_specs=vmem,
        scratch_shapes=[
            pltpu.VMEM((rows, width), jnp.bfloat16),
            pltpu.VMEM((depth, hidden), jnp.float32),
            pltpu.VMEM((hidden, cols), jnp.float32),
            pltpu.VMEM((depth, wide), jnp.bfloat16),
            pltpu.VMEM((wide, cols), jnp.bfloat16),
            pltpu.VMEM((width, wide), jnp.bfloat16),
            pltpu.VMEM((nz * NY, wide, pair), jnp.bfloat16),
            pltpu.VMEM((rows, width), jnp.bfloat16),
            pltpu.VMEM((2 * rows, wide), jnp.bfloat16),
            pltpu.VMEM((4, 2, rows, pair), jnp.bfloat16),
            pltpu.VMEM((4, 2, rows, pair), jnp.bfloat16),
            pltpu.VMEM((4, rows, pair), jnp.bfloat16),
            pltpu.VMEM((4, rows, pair), jnp.bfloat16),
            pltpu.VMEM((4, rows, pair), jnp.float32),
            pltpu.VMEM((rows, pair), jnp.float32),
            pltpu.SemaphoreType.DMA((ways,)),
            pltpu.SemaphoreType.DMA((ways,)),
            pltpu.SemaphoreType.DMA((3,)),
        ],
        compiler_params=pltpu.CompilerParams(
            collective_id=0, has_side_effects=True, vmem_limit_bytes=60 * 1024 * 1024
        ),
    )(tokens, norm_gain[None], up_scale[None], up_weight, down_weight, down_scale[None])


def solution(mesh):
    in_specs = (P("fs", None), P(), P("fs", "tp"), P("tp"), P("tp", "fs"), P("fs"))
    out_specs = P("fs", "tp")
    nz = mesh.shape["fs"] // (NX * NY)
    local = fused if nz == 4 and mesh.shape["tp"] == 2 else plain
    return jax.shard_map(local, mesh=mesh, in_specs=in_specs, out_specs=out_specs, check_vma=False)
```

```python
import jax
import jax.numpy as jnp
from jax import lax
from jax.experimental import pallas as pl
from jax.experimental.pallas import tpu as pltpu
from jax.sharding import PartitionSpec as P

epsilon = 1e-06


def normalise(tokens, norm_gain):
    floats = tokens.astype(jnp.float32)
    inverse = lax.rsqrt(jnp.mean(floats * floats, axis=-1, keepdims=True) + epsilon)
    return (floats * inverse * norm_gain).astype(jnp.bfloat16)


def plain(tokens, norm_gain, up_weight, up_scale, down_weight, down_scale):
    normed = normalise(tokens, norm_gain)
    up_whole = lax.all_gather(up_weight.astype(jnp.bfloat16), "fs", axis=0, tiled=True)
    up_pre = jnp.dot(normed, up_whole, preferred_element_type=jnp.float32)
    scaled = (down_weight * down_scale).astype(jnp.bfloat16)
    down_whole = lax.all_gather(scaled, "fs", axis=1, tiled=True)
    hidden = jnp.square(jax.nn.relu(up_pre * up_scale)).astype(jnp.bfloat16)
    partial_value = jnp.dot(hidden, down_whole, preferred_element_type=jnp.float32)
    return lax.psum_scatter(
        partial_value.astype(jnp.bfloat16), "tp", scatter_dimension=1, tiled=True
    )


NX, NY = 2, 2
order = (0, 1, 3, 2)


def kernel(tok_ref, gain_hbm, s_hbm, up_ref, down_ref, dscale_hbm, out_ref,
           gain_ref, s_ref, dscale_ref, x_buf, u_in, d_in, u_send, d_send, u_buf, d_buf, t_buf, h_buf, ssend, srecv,
           xsend, xrecv, keep, part, send_sems, recv_sems, local_sems):
    me = lax.axis_index("fs")
    c = lax.axis_index("tp")
    x = lax.rem(me, NX)
    y = lax.rem(me // NX, NY)
    z = me // (NX * NY)
    side = lax.rem(z, 2)
    rows = x_buf.shape[0]
    depth = u_send.shape[0]
    wide = u_send.shape[1]
    cols = d_send.shape[1]
    pair = NX * cols
    part_rows = rows // 2

    def fs_of(zz, yy, xx):
        return (zz * NY + yy) * NX + xx

    def level(k):
        return {0: z, 1: z + 1 - 2 * side, 2: lax.rem(z + 2, 4), 3: 3 - z}[k]

    target = {
        **{k: {"fs": fs_of(level(k), y, x), "tp": c} for k in (1, 2, 3)},
        "y": {"fs": fs_of(z, 1 - y, x), "tp": c},
        "x": {"fs": fs_of(z, y, 1 - x), "tp": c},
        "c": {"fs": me, "tp": 1 - c},
    }
    peer = 1

    mine_rows = pl.ds(pl.multiple_of(c * part_rows, part_rows), part_rows)
    other_rows = pl.ds(pl.multiple_of((1 - c) * part_rows, part_rows), part_rows)
    at_own = pl.ds(pl.multiple_of(side * wide, wide), wide)
    at_other = pl.ds(pl.multiple_of((1 - side) * wide, wide), wide)
    local = [
        pltpu.make_async_copy(up_ref.at[:, at_own], u_in.at[:, at_own], local_sems.at[0]),
        pltpu.make_async_copy(up_ref.at[:, at_other], u_in.at[:, at_other], local_sems.at[3]),
        pltpu.make_async_copy(tok_ref, x_buf, local_sems.at[1]),
        pltpu.make_async_copy(down_ref, d_in, local_sems.at[2]),
        pltpu.make_async_copy(gain_hbm, gain_ref, local_sems.at[4]),
        pltpu.make_async_copy(s_hbm, s_ref, local_sems.at[5]),
        pltpu.make_async_copy(dscale_hbm, dscale_ref, local_sems.at[6]),
    ]
    for copy in local:
        copy.start()

    barrier = pltpu.get_barrier_semaphore()
    for where in target.values():
        pl.semaphore_signal(barrier, inc=1, device_id=where, device_id_type=pl.DeviceIdType.MESH)

    slots, started, guarded = {}, [], []

    def copy_of(key, src, dst, way, sent=None):
        n = slots.setdefault(key, len(slots))
        m = n if sent is None else slots.setdefault(sent, len(slots))
        return pltpu.make_async_remote_copy(
            src_ref=src, dst_ref=dst, send_sem=send_sems.at[m], recv_sem=recv_sems.at[n],
            device_id=target[way], device_id_type=pl.DeviceIdType.MESH)

    def launch(key, src, dst, way):
        copy = copy_of(key, src, dst, way)
        copy.start()
        started.append(copy)

    def arrive(key, dst, way="x"):
        copy_of(key, dst, dst, way).wait_recv()

    def block(kind, k, px, py, half=None):
        zz, yy = level(k), lax.rem(y + py, NY)
        xx = lax.rem(x + px, NX)
        if kind == "U":
            size = depth if half is None else depth // 2
            at = fs_of(zz, yy, xx) * depth + (0 if half in (None, 0) else size)
            return u_buf.at[pl.ds(pl.multiple_of(at, size), size), :]
        size = wide if half is None else wide // 2
        at = 0 if half in (None, 0) else size
        return d_buf.at[zz * NY + yy, pl.ds(at, size), pl.ds(pl.multiple_of(xx * cols, cols), cols)]

    own = {kind: block(kind, 0, 0, 0) for kind in "UD"}
    other = {"U": u_send, "D": d_send}

    inner = (z + 1) // 2 == 1
    outer = jnp.logical_not(inner)

    def launch_if(where, copy):
        @pl.when(where)
        def _():
            copy.start()

        guarded.append((where, copy))

    def column(kind, k, where=None):
        copy = copy_of((kind, k, 0, 0, None), own[kind] if k == 2 else other[kind], own[kind], k)
        if where is None:
            copy.start()
            started.append(copy)
        else:
            launch_if(where, copy)

    def relay(kind):
        take(kind, 1, 0, 0)
        ref = block(kind, 1, 0, 0)
        launch_if(inner, copy_of((kind, 3, 0, 0, None), ref, ref, 2, ("R", kind)))

    def take(kind, k, px, py, half=None):
        arrive((kind, k, px, py, half), block(kind, k, px, py, half))

    def share(kind, k):
        if k > 1:
            take(kind, k, 0, 0)
        ref = block(kind, k, 0, 0)
        launch((kind, k, 1, 0, None), ref, ref, "x")
        launch((kind, k, 0, 1, None), ref, ref, "y")

    def cross(kind, k):
        for px, py, way, half in ((1, 0, "y", 0), (0, 1, "x", 1)):
            take(kind, k, px, py)
            ref = block(kind, k, px, py, half)
            launch((kind, k, 1, 1, half), ref, ref, way)

    def corner(kind, k):
        take(kind, k, 1, 1, 0)
        take(kind, k, 1, 1, 1)

    local[0].wait()
    own["U"][...] = u_in[:, at_own].astype(jnp.bfloat16)
    local[1].wait()
    u_send[...] = u_in[:, at_other].astype(jnp.bfloat16)
    pl.semaphore_wait(barrier, len(target))
    column("U", 1)
    share("U", 0)
    column("U", 3, inner)
    column("U", 2, outer)

    for copy in local[3:]:
        copy.wait()
    d_send[...] = (d_in[at_other, :] * dscale_ref[...]).astype(jnp.bfloat16)
    own["D"][...] = (d_in[at_own, :] * dscale_ref[...]).astype(jnp.bfloat16)

    step = 16

    def normalise_rows(base):
        @pl.loop(0, part_rows // step)
        def _(i):
            r = pl.ds(pl.multiple_of(base + i * step, step), step)
            floats = x_buf[r, :].astype(jnp.float32)
            inverse = lax.rsqrt(jnp.mean(floats * floats, axis=-1, keepdims=True) + epsilon)
            x_buf[r, :] = (floats * inverse * gain_ref[...]).astype(jnp.bfloat16)

    local[2].wait()
    normalise_rows(c * part_rows)
    column("D", 1)
    launch(("T", "x"), x_buf.at[mine_rows, :], t_buf.at[mine_rows, :], peer)
    normalise_rows((1 - c) * part_rows)

    relay("U")
    share("U", 1)
    column("U", 2, inner)
    cross("U", 0)
    cross("U", 1)
    share("D", 0)
    share("U", 3)
    share("U", 2)
    cross("U", 3)
    relay("D")
    column("D", 3, inner)
    column("D", 2)
    cross("U", 2)
    cross("D", 0)
    share("D", 1)
    for k in order:
        corner("U", k)

    tile_m, tile_n = part_rows, min(512, wide)
    chunks = wide // tile_n

    def up_part(src, base, first, count, jfirst=0, jcount=chunks):
        @pl.loop(jfirst, jfirst + jcount)
        def _(j):
            at = pl.ds(pl.multiple_of(j * tile_n, tile_n), tile_n)
            at_s = pl.ds(pl.multiple_of(side * wide + j * tile_n, tile_n), tile_n)

            for i in range(count):
                r = pl.multiple_of(first + i * tile_m, tile_m)
                pre = jnp.dot(src[pl.ds(r, tile_m), :], u_buf[:, at],
                              preferred_element_type=jnp.float32)
                act = jnp.square(jnp.maximum(pre * s_ref[:, at_s], 0.0))
                h_buf[pl.ds(base + r, tile_m), at] = act.astype(jnp.bfloat16)

    up_part(x_buf, 0, 0, 2)
    share("D", 3)
    arrive(("T", "x"), t_buf.at[mine_rows, :])
    launch(("T", "c"), t_buf.at[mine_rows, :], t_buf.at[mine_rows, :], "c")
    up_part(t_buf, rows, c * part_rows, 1)
    arrive(("T", "c"), t_buf.at[other_rows, :])
    up_part(t_buf, rows, (1 - c) * part_rows, 1)
    cross("D", 1)

    pending = []

    def stage(k, py):
        j = order.index(k)
        zz, yy = level(k), lax.rem(y + py, NY)
        zy = zz * NY + yy
        n = (j % 2) * 2 + py
        met = (n + 2) % 4
        mine = zz // 2 == c

        def sum_of(half):
            return copy_of(("S", n, half), ssend.at[n, half], srecv.at[n, half], "c")

        def cross_of():
            return copy_of(("X", met), xsend.at[n], xrecv.at[met], peer)

        def land_of():
            return copy_of(("X", n), xsend.at[n], xrecv.at[n], peer)

        for half, base in ((0, rows), (1, 0)):
            part[half] = jnp.dot(h_buf[pl.ds(base, rows), :], d_buf[zy],
                                 preferred_element_type=jnp.float32)

            @pl.when(jnp.logical_not(mine))
            def _():
                ssend[n, half] = part[half].astype(jnp.bfloat16)
                sum_of(half).start()

        @pl.when(mine)
        def _():
            sum_of(0).wait_recv()
            xsend[n] = (part[0] + srecv[n, 0].astype(jnp.float32)).astype(jnp.bfloat16)
            cross_of().start()
            sum_of(1).wait_recv()
            keep[n] = part[1] + srecv[n, 1].astype(jnp.float32)

        def finish():
            @pl.when(mine)
            def _():
                at = pl.multiple_of((lax.rem(zz, 2) * NY + yy) * pair, pair)
                land_of().wait_recv()
                out_ref[:, pl.ds(at, pair)] = (keep[n] + xrecv[n].astype(jnp.float32)
                                               ).astype(out_ref.dtype)

        def drain():
            @pl.when(mine)
            def _():
                cross_of().wait_send()

            @pl.when(jnp.logical_not(mine))
            def _():
                for half in range(2):
                    sum_of(half).wait_send()

        pending.append((finish, drain))

    stage(0, 0)
    share("D", 2)
    corner("D", 0)
    stage(0, 1)
    stage(1, 0)
    cross("D", 3)
    corner("D", 1)
    stage(1, 1)
    stage(3, 0)
    cross("D", 2)
    stage(2, 0)
    corner("D", 3)
    stage(3, 1)
    for finish, _ in pending[:4]:
        finish()
    corner("D", 2)
    stage(2, 1)
    for finish, _ in pending[4:6]:
        finish()
    pending[7][0]()
    pending[6][0]()
    for _, drain in pending:
        drain()
    for copy in started:
        copy.wait_send()
    for where, copy in guarded:
        @pl.when(where)
        def _(copy=copy):
            copy.wait_send()


def fused(tokens, norm_gain, up_weight, up_scale, down_weight, down_scale):
    rows, width = tokens.shape
    depth, hidden = up_weight.shape
    cols = down_weight.shape[1]
    wide = hidden // 2
    nz = 4
    pair = NX * cols
    ways = 2 * (2 * (nz - 1) + 6 * nz) + 2 + 40
    vmem = pl.BlockSpec(memory_space=pltpu.VMEM)
    hbm = pl.BlockSpec(memory_space=pltpu.HBM)
    return pl.pallas_call(
        kernel,
        out_shape=jax.ShapeDtypeStruct((rows, width // 2), jnp.bfloat16),
        in_specs=[hbm] * 6,
        out_specs=vmem,
        scratch_shapes=[
            pltpu.VMEM((1, width), jnp.float32),
            pltpu.VMEM((1, hidden), jnp.float32),
            pltpu.VMEM((1, cols), jnp.float32),
            pltpu.VMEM((rows, width), jnp.bfloat16),
            pltpu.VMEM((depth, hidden), jnp.float32),
            pltpu.VMEM((hidden, cols), jnp.float32),
            pltpu.VMEM((depth, wide), jnp.bfloat16),
            pltpu.VMEM((wide, cols), jnp.bfloat16),
            pltpu.VMEM((width, wide), jnp.bfloat16),
            pltpu.VMEM((nz * NY, wide, pair), jnp.bfloat16),
            pltpu.VMEM((rows, width), jnp.bfloat16),
            pltpu.VMEM((2 * rows, wide), jnp.bfloat16),
            pltpu.VMEM((4, 2, rows, pair), jnp.bfloat16),
            pltpu.VMEM((4, 2, rows, pair), jnp.bfloat16),
            pltpu.VMEM((4, rows, pair), jnp.bfloat16),
            pltpu.VMEM((4, rows, pair), jnp.bfloat16),
            pltpu.VMEM((4, rows, pair), jnp.float32),
            pltpu.VMEM((2, rows, pair), jnp.float32),
            pltpu.SemaphoreType.DMA((ways,)),
            pltpu.SemaphoreType.DMA((ways,)),
            pltpu.SemaphoreType.DMA((7,)),
        ],
        compiler_params=pltpu.CompilerParams(
            collective_id=0, has_side_effects=True, vmem_limit_bytes=52 * 1024 * 1024
        ),
    )(tokens, norm_gain[None], up_scale[None], up_weight, down_weight, down_scale[None])


def solution(mesh):
    in_specs = (P("fs", None), P(), P("fs", "tp"), P("tp"), P("tp", "fs"), P("fs"))
    out_specs = P("fs", "tp")
    nz = mesh.shape["fs"] // (NX * NY)
    local = fused if nz == 4 and mesh.shape["tp"] == 2 else plain
    return jax.shard_map(local, mesh=mesh, in_specs=in_specs, out_specs=out_specs, check_vma=False)
```
